32 devices in a mesh: sp: 16 (over z, y, core), tp: 2 (over x).
Axes of the slice: x: 2, y: 2, z: 4, core: 2. Of those that a mesh axis runs over, the one named last changes fastest.
Arguments:
- block_input: bfloat16 [6144, 2048], P('sp'), may hold values from -6 to 6
- proj_x: bfloat16 [2048, 1024], P(None, 'tp'), may hold values from -0.125 to 0.125
- proj_gate: bfloat16 [2048, 1024], P(None, 'tp'), may hold values from -0.125 to 0.125
- conv_taps: float32 [4, 1024], P(None, 'tp'), may hold values from -3 to 3
- gate_a: bfloat16 [16, 64, 64], P('tp'), may hold values from -0.75 to 0.75
- gate_in: bfloat16 [16, 64, 64], P('tp'), may hold values from -0.75 to 0.75
- decay_param: float32 [1024], P('tp'), may hold values from 3 to 30
- log_jump: float32 [6144, 1024], P('sp', 'tp'), may hold values from -1 to 0, as said below
- out_grad: bfloat16 [6144, 1024], P('sp', 'tp'), may hold values from -6 to 6
Outputs:
- grad_input: bfloat16 [6144, 2048], P(('sp', 'tp'))
- grad_proj: float32 [2048, 1024], P('sp', 'tp')
The draws below stay inside these ranges and needn't reach their ends.
Inputs may be any that keep to these rules, and one draw needn't show every extreme that they name: `log_jump`: strictly negative.
All inputs are finite; a program needn't handle non-finite values.
Results may differ from the reference program's by a relative error of at most 0.015.
Values may be sent and summed in bfloat16 or wider, within the bound.
A program may use at most 64 MiB of HBM per device.

```python
import math
import jax
import jax.numpy as jnp
from jax import lax

D = 2048
RECUR_CHANNELS = 1024
BLOCK = 64
TAPS = 4
TOK_DEV = 384
BLOCKS = 16
SEQUENCE_TOKENS = 6144
N_TP = 2


def draw_decay_param(key, part):
    key_kind = jax.random.fold_in(key, 11)
    key_fast = jax.random.fold_in(key, 12)
    key_slow = jax.random.fold_in(key, 13)
    fast_share = 0.5
    is_fast = jax.random.uniform(key_kind, (RECUR_CHANNELS,), jnp.float32) < fast_share
    fast_rate = jnp.exp(jax.random.uniform(key_fast, (RECUR_CHANNELS,), jnp.float32, math.log(1.0 / 400.0), math.log(1.0 / 120.0)))
    slow_rate = jax.random.uniform(key_slow, (RECUR_CHANNELS,), jnp.float32, 0.05, 0.3) * math.log(10.0) / (4.0 * SEQUENCE_TOKENS)
    rate = jnp.where(is_fast, fast_rate, slow_rate)
    return (-rate - jnp.log(-jnp.expm1(-rate))).astype(jnp.float32)


def draw_log_jump(key, part):
    key_block = jax.random.fold_in(key, 21)
    random_key_mask = jax.random.fold_in(key, 22)
    key_depth = jax.random.fold_in(key, 23)
    block_count = SEQUENCE_TOKENS // TOK_DEV
    spread = math.log(2.0)
    factor = jnp.exp(jax.random.uniform(key_block, (block_count, RECUR_CHANNELS), jnp.float32, -spread, spread))
    base_offset = -math.log(10.0) / (8.0 * SEQUENCE_TOKENS) * jnp.repeat(factor, TOK_DEV, axis=0)
    spike_mask = jax.random.uniform(random_key_mask, (SEQUENCE_TOKENS, RECUR_CHANNELS), jnp.float32) < 2.0 / SEQUENCE_TOKENS
    layer_depth = jnp.log(jax.random.uniform(key_depth, (SEQUENCE_TOKENS, RECUR_CHANNELS), jnp.float32, 0.55, 0.8))
    return (base_offset + jnp.where(spike_mask, layer_depth, 0.0)).astype(jnp.float32)


def spiked(drawn, own_key, source, target, parts, factor):
    owner, partner = [(jnp.arange(drawn.shape[dim]) // (drawn.shape[dim] // parts)).reshape([-1 if axis == dim else 1 for axis in range(drawn.ndim)]) for dim in (source, target)]
    chosen = jax.random.permutation(own_key, parts)[partner]
    strong = (owner == chosen) | (owner == (partner + parts // 2) % parts)
    return jnp.where(strong, factor * drawn, drawn)


def levels(stream_key, dims, pieces, smallest, high):
    gain = 1.0
    for axis_at, shards_of in pieces:
        steps = jax.random.uniform(jax.random.fold_in(jax.random.fold_in(stream_key, 6), axis_at), (shards_of,), jnp.float32, smallest / len(pieces), high / len(pieces))
        gain = gain * jnp.repeat(jnp.exp(steps), dims[axis_at] // shards_of).reshape((-1,) + (1,) * (len(dims) - 1 - axis_at))
    return gain


def centred(stream_key, shape, scale, bound, split=(), held_as=jnp.bfloat16):
    result = jax.random.normal(stream_key, shape, jnp.float32) * scale
    if len(split) > 0:
        result = levels(stream_key, shape, split, -0.22, 0.18) * result
    return jnp.clip(result, min=-bound, max=bound).astype(held_as)


def bell_draw_with(own_key, extent, scale, reach, split, heavy, held_as=jnp.bfloat16):
    array = scale * jax.random.normal(own_key, extent, jnp.float32)
    if split:
        array = array * levels(own_key, extent, split, -0.22, 0.18)
    return jnp.clip(spiked(array, jax.random.fold_in(own_key, 3), *heavy), -reach, reach).astype(held_as)


def setup_inputs(seed: int = 0) -> dict:
    key_of = jax.random.split(jax.random.key(seed), 10)
    block_input = bell_draw_with(key_of[0], (SEQUENCE_TOKENS, D), 1.0, 6.0, ((0, 16),), (0, 1, 16, 2.0))
    proj_x = centred(key_of[1], (D, RECUR_CHANNELS), D ** -0.5, 0.125, ((1, 2),))
    proj_gate = centred(key_of[2], (D, RECUR_CHANNELS), D ** -0.5, 0.125, ((1, 2),))
    conv_taps = centred(key_of[3], (TAPS, RECUR_CHANNELS), TAPS ** -0.5, 3.0, ((1, 2),), jnp.float32)
    gate_a = centred(key_of[4], (BLOCKS, BLOCK, BLOCK), BLOCK ** -0.5, 0.75, ((0, 2),))
    gate_in = centred(key_of[5], (BLOCKS, BLOCK, BLOCK), BLOCK ** -0.5, 0.75, ((0, 2),))
    decay_param = draw_decay_param(jax.random.fold_in(key_of[9], 71), 0)
    log_jump = draw_log_jump(jax.random.fold_in(key_of[9], 71), 0)
    out_grad = centred(key_of[8], (SEQUENCE_TOKENS, RECUR_CHANNELS), 1.0, 6.0, ((0, 16), (1, 2)))
    return {"block_input": block_input, "proj_x": proj_x, "proj_gate": proj_gate, "conv_taps": conv_taps, "gate_a": gate_a, "gate_in": gate_in, "decay_param": decay_param, "log_jump": log_jump, "out_grad": out_grad}


gate_power = 8.0

def combine(earlier, later):
    return (earlier[0] * later[0], later[0] * earlier[1] + later[1])

def reference(block_input, proj_x, proj_gate, conv_taps, gate_a, gate_in, decay_param, log_jump, out_grad):
    branch = jnp.dot(block_input, proj_x, preferred_element_type=jnp.float32).astype(jnp.bfloat16)
    gate_pre = jnp.dot(block_input, proj_gate, preferred_element_type=jnp.float32).astype(jnp.bfloat16)
    padded = jnp.pad(branch.astype(jnp.float32), ((TAPS - 1, 0), (0, 0)))
    mixed_sum = jnp.zeros((SEQUENCE_TOKENS, RECUR_CHANNELS), jnp.float32)
    for offset in range(TAPS):
        mixed_sum = mixed_sum + conv_taps[offset][None, :] * padded[offset:offset + SEQUENCE_TOKENS]
    mixed = mixed_sum.astype(jnp.bfloat16)
    mixed_f = mixed.astype(jnp.float32)
    mixed_blocks = mixed_f.reshape(SEQUENCE_TOKENS, BLOCKS, BLOCK)
    rec_gate = jax.nn.sigmoid(jnp.einsum('tbi,bij->tbj', mixed_blocks, gate_a.astype(jnp.float32)).reshape(SEQUENCE_TOKENS, RECUR_CHANNELS))
    in_gate = jax.nn.sigmoid(jnp.einsum('tbi,bij->tbj', mixed_blocks, gate_in.astype(jnp.float32)).reshape(SEQUENCE_TOKENS, RECUR_CHANNELS))
    log_sig = jax.nn.log_sigmoid(decay_param)
    log_decay = gate_power * rec_gate * log_sig[None, :] + log_jump
    decays = jnp.exp(log_decay)
    square_decay = jnp.exp(2.0 * log_decay)
    norm_factor = jnp.sqrt(-jnp.expm1(2.0 * log_decay))
    drive = norm_factor * in_gate * mixed_f
    _, hidden = lax.associative_scan(combine, (decays, drive), axis=0)
    activation, pullback = jax.vjp(jax.nn.gelu, gate_pre.astype(jnp.float32))
    grad_out = out_grad.astype(jnp.float32)
    grad_hidden = grad_out * activation
    next_decay = jnp.concatenate([decays[1:], jnp.ones((1, RECUR_CHANNELS), jnp.float32)], axis=0)
    _, flipped = lax.associative_scan(combine, (next_decay[::-1], grad_hidden[::-1]), axis=0)
    grad_state = flipped[::-1]
    hidden_prev = jnp.concatenate([jnp.zeros((1, RECUR_CHANNELS), jnp.float32), hidden[:-1]], axis=0)
    grad_log = grad_state * hidden_prev * decays - grad_state * in_gate * mixed_f * square_decay / norm_factor
    grad_pre_a = (grad_log * gate_power * log_sig[None, :] * rec_gate * (1.0 - rec_gate)).astype(jnp.bfloat16)
    grad_pre_in = (grad_state * norm_factor * mixed_f * in_gate * (1.0 - in_gate)).astype(jnp.bfloat16)
    back_a = jnp.einsum('tbj,bij->tbi', grad_pre_a.astype(jnp.float32).reshape(SEQUENCE_TOKENS, BLOCKS, BLOCK), gate_a.astype(jnp.float32))
    back_in = jnp.einsum('tbj,bij->tbi', grad_pre_in.astype(jnp.float32).reshape(SEQUENCE_TOKENS, BLOCKS, BLOCK), gate_in.astype(jnp.float32))
    grad_mixed = grad_state * norm_factor * in_gate + (back_a + back_in).reshape(SEQUENCE_TOKENS, RECUR_CHANNELS)
    padded_grad = jnp.pad(grad_mixed, ((0, TAPS - 1), (0, 0)))
    branch_sum = jnp.zeros((SEQUENCE_TOKENS, RECUR_CHANNELS), jnp.float32)
    for offset in range(TAPS):
        start = TAPS - 1 - offset
        branch_sum = branch_sum + conv_taps[offset][None, :] * padded_grad[start:start + SEQUENCE_TOKENS]
    grad_branch = branch_sum.astype(jnp.bfloat16)
    stored_hidden = lax.optimization_barrier(hidden.astype(jnp.bfloat16)).astype(jnp.float32)
    grad_gate = pullback(grad_out * stored_hidden)[0].astype(jnp.bfloat16)
    grad_proj = lax.dot_general(block_input, grad_branch, (((0,), (0,)), ((), ())), preferred_element_type=jnp.float32)
    group_width = RECUR_CHANNELS // N_TP
    total = jnp.zeros((SEQUENCE_TOKENS, D), jnp.float32)
    for group in range(N_TP):
        lower = group * group_width
        upper = lower + group_width
        partial_sum = lax.dot_general(grad_branch[:, lower:upper], proj_x[:, lower:upper], (((1,), (1,)), ((), ())), preferred_element_type=jnp.float32)
        partial_sum = partial_sum + lax.dot_general(grad_gate[:, lower:upper], proj_gate[:, lower:upper], (((1,), (1,)), ((), ())), preferred_element_type=jnp.float32)
        total = total + lax.optimization_barrier(partial_sum.astype(jnp.bfloat16)).astype(jnp.float32)
    return (total.astype(jnp.bfloat16), grad_proj)
```

```python
import functools

import jax
import jax.numpy as jnp
from jax import lax
from jax.experimental import pallas as pl
from jax.experimental.pallas import tpu as pltpu
from jax.sharding import PartitionSpec as P

gate_power = 8.0
LANES = 128
SEGS = 8
HALO = 16
GELU_C = 0.7978845608028654
GELU_K = 0.044715
F32 = jnp.float32
BF16 = jnp.bfloat16
MESH = pl.DeviceIdType.MESH


def neg_expm1(y, ey):
    p = 1.0 + y * (1.0 / 8.0)
    for k in range(7, 1, -1):
        p = 1.0 + y * (1.0 / k) * p
    return jnp.where(y > -0.5, -y * p, 1.0 - ey)


def log_sigmoid(x):
    e = jnp.exp(-jnp.abs(x))
    s = e / (2.0 + e)
    s2 = s * s
    p = jnp.full_like(s, 1.0 / 17.0)
    for k in range(15, 0, -2):
        p = p * s2 + 1.0 / k
    return jnp.minimum(x, 0.0) - 2.0 * s * p


def dot(a, b, dims=((1,), (0,))):
    return lax.dot_general(a, b, (dims, ((), ())), preferred_element_type=F32)


def factor(n):
    bits, last = 0, n
    while last > 4 and last % 2 == 0:
        last //= 2
        bits += 1
    return last, bits


def bitrev(v, bits):
    out = 0
    for i in range(bits):
        out = out * 2 + (v >> i) % 2
    return out


def kernel(
    n_sp, n_tp, x_hbm, wx_hbm, wg_hbm, taps, ga, gi, dp, lj_hbm, og_hbm,
    gin_out, gproj_out,
    xs, wx, wg, lj, og, gt, br, mix, mixb, bda, bdi, rec, ing, dec, nrm, us, ps, gs, qs,
    cs, rs, sbuf, rbuf, pab, pib, gg, gm, gb, acc, tsend, trecv, part, srecv, sacc, lrecv,
    loc_sem, halo_sem, msend_sem, mrecv_sem, head_sem, tsend_sem, trecv_sem, ssend_sem,
    srecv_sem, lsend_sem, lrecv_sem,
):
    me = lax.axis_index("sp")
    tp = lax.axis_index("tp")
    rows, chans = og.shape
    depth = wx.shape[0]
    nq = chans // LANES
    taps_n = taps.shape[0]
    block = ga.shape[1]
    seg = rows // SEGS
    last, bits = factor(n_sp)
    per_last = n_sp // last

    barrier = pltpu.get_barrier_semaphore()
    for k in range(1, n_sp):
        pl.semaphore_signal(
            barrier, inc=1, device_id={"sp": lax.rem(me + k, n_sp)}, device_id_type=MESH
        )
    for k in range(1, n_tp):
        pl.semaphore_signal(
            barrier, inc=1, device_id={"tp": lax.rem(tp + k, n_tp)}, device_id_type=MESH
        )
    loads = []
    for i, (src, dst) in enumerate(
        ((x_hbm, xs.at[pl.ds(HALO, rows)]), (wg_hbm, wg), (wx_hbm, wx), (lj_hbm, lj), (og_hbm, og))
    ):
        c = pltpu.make_async_copy(src, dst, loc_sem.at[i])
        c.start()
        loads.append(c)

    gw = bda.shape[1]
    spread = (
        lax.rem(lax.broadcasted_iota(jnp.int32, (block, gw), 1), block)
        == lax.broadcasted_iota(jnp.int32, (block, gw), 0)
    ).astype(F32).astype(BF16)
    keep = lax.rem(lax.broadcasted_iota(jnp.int32, (chans, gw), 0), gw) // block == (
        lax.broadcasted_iota(jnp.int32, (chans, gw), 1) // block
    )
    for src, dst in ((ga, bda), (gi, bdi)):
        flat = src[...].reshape(chans, block)
        dst[...] = jnp.where(keep, dot(flat, spread), 0.0).astype(BF16)

    loads[0].wait()
    pl.semaphore_wait(barrier, n_sp - 1 + n_tp - 1)
    halo = pltpu.make_async_remote_copy(
        src_ref=xs.at[pl.ds(rows, HALO)], dst_ref=xs.at[pl.ds(0, HALO)],
        send_sem=halo_sem.at[0], recv_sem=halo_sem.at[1],
        device_id={"sp": lax.rem(me + 1, n_sp)}, device_id_type=MESH,
    )
    halo.start()
    loads[1].wait()
    pre = dot(xs[pl.ds(HALO, rows), :], wg[...]).astype(BF16).astype(F32)
    for q in range(nq):
        gt[q] = pre[:, q * LANES : (q + 1) * LANES]
    loads[2].wait()
    halo.wait_recv()
    pre = dot(xs[...], wx[...]).astype(BF16).astype(F32)
    for q in range(nq):
        br[q] = pre[:, q * LANES : (q + 1) * LANES]
    first = me == 0
    for q in range(nq):
        br[q, pl.ds(0, HALO), :] = jnp.where(first, 0.0, br[q, pl.ds(0, HALO), :])

    step = 128 if rows % 128 == 0 else rows
    for q in range(nq):
        lanes = slice(q * LANES, (q + 1) * LANES)
        for r in range(0, rows, step):
            total = jnp.zeros((step, LANES), F32)
            for j in range(taps_n):
                off = HALO - taps_n + 1 + j + r
                total = total + taps[j : j + 1, lanes] * br[q, off : off + step, :]
            half = total.astype(BF16)
            mixb[r : r + step, lanes] = half
            mix[q, r : r + step, :] = half.astype(F32)

    for src, dst in ((bda, rec), (bdi, ing)):
        for g in range(chans // gw):
            cols = slice(g * gw, (g + 1) * gw)
            pre = dot(mixb[:, cols], src[cols, :])
            for q in range(gw // LANES):
                dst[g * (gw // LANES) + q] = pre[:, q * LANES : (q + 1) * LANES]

    loads[3].wait()
    loads[4].wait()
    sub = 64 if rows % 64 == 0 else rows
    log_sig = log_sigmoid(dp[...])
    for q in range(nq):
        lanes = slice(q * LANES, (q + 1) * LANES)
        scale = gate_power * log_sig[:, lanes]

        def gates(i, carry, q=q, lanes=lanes, scale=scale):
            r = pl.ds(pl.multiple_of(i * sub, sub), sub)
            rg = jax.nn.sigmoid(rec[q, r, :])
            ig = jax.nn.sigmoid(ing[q, r, :])
            log_decay = rg * scale + lj[r, lanes]
            a = jnp.exp(log_decay)
            v = neg_expm1(2.0 * log_decay, a * a)
            norm = jnp.sqrt(v)
            rec[q, r, :] = rg
            ing[q, r, :] = ig
            dec[q, r, :] = a
            nrm[q, r, :] = norm
            us[q, r, :] = norm * ig * mix[q, r, :]
            z = gt[q, r, :]
            t = jnp.tanh(GELU_C * (z + GELU_K * (z * z * z)))
            gs[q, r, :] = og[r, lanes].astype(F32) * (0.5 * z * (1.0 + t))
            return carry

        lax.fori_loop(0, rows // sub, gates, 0)

    def scan(i, carry):
        out = []
        for q in range(nq):
            h, p, g, w = carry[q]
            f = pl.ds(i, SEGS, stride=seg)
            b = pl.ds(seg - 1 - i, SEGS, stride=seg)
            a = dec[q, f, :]
            u = a * h
            h = u + us[q, f, :]
            p = a * p
            us[q, f, :] = u
            ps[q, f, :] = p
            g = gs[q, b, :] + g
            gs[q, b, :] = g
            qs[q, b, :] = w
            a = dec[q, b, :]
            out.append((h, p, a * g, a * w))
        return tuple(out)

    zero = jnp.zeros((SEGS, LANES), F32)
    one = jnp.ones((SEGS, LANES), F32)
    ends = lax.fori_loop(0, seg, scan, tuple((zero, one, zero, one) for _ in range(nq)), unroll=2)
    for q in range(nq):
        h, p, g, _ = ends[q]
        fwd = jnp.zeros((1, LANES), F32)
        bwd = jnp.zeros((1, LANES), F32)
        prod = jnp.ones((1, LANES), F32)
        for s in range(SEGS):
            e = SEGS - 1 - s
            fwd = p[s : s + 1] * fwd + h[s : s + 1]
            bwd = p[e : e + 1] * bwd + g[e : e + 1]
            prod = prod * p[s : s + 1]
        sbuf[0, q : q + 1, :] = prod
        sbuf[1, q : q + 1, :] = prod
        sbuf[0, nq + q : nq + q + 1, :] = fwd
        sbuf[1, nq + q : nq + q + 1, :] = bwd

    sent = []
    for k in range(1, n_sp):
        peer = lax.rem(me + k, n_sp)
        c = pltpu.make_async_remote_copy(
            src_ref=sbuf.at[jnp.where(peer > me, 0, 1)], dst_ref=rbuf.at[k],
            send_sem=msend_sem.at[k], recv_sem=mrecv_sem.at[k],
            device_id={"sp": peer}, device_id_type=MESH,
        )
        c.start()
        sent.append(c)
    for c in sent:
        c.wait_recv()
    fwd = jnp.zeros((nq, LANES), F32)
    bwd = jnp.zeros((nq, LANES), F32)
    for k in range(n_sp - 1, 0, -1):
        fwd = jnp.where(me >= k, rbuf[k, 0:nq, :] * fwd + rbuf[k, nq : 2 * nq, :], fwd)
    for k in range(1, n_sp):
        bwd = jnp.where(me < k, rbuf[k, 0:nq, :] * bwd + rbuf[k, nq : 2 * nq, :], bwd)
    for q in range(nq):
        h, p, g, _ = ends[q]
        c = fwd[q : q + 1]
        d = bwd[q : q + 1]
        for s in range(SEGS):
            e = SEGS - 1 - s
            cs[q, s : s + 1, :] = c
            rs[q, e : e + 1, :] = d
            c = p[s : s + 1] * c + h[s : s + 1]
            d = p[e : e + 1] * d + g[e : e + 1]

    for q in range(nq):
        lanes = slice(q * LANES, (q + 1) * LANES)
        scale = gate_power * log_sig[:, lanes]

        def grads(s, carry, q=q, lanes=lanes, scale=scale):
            r = pl.ds(pl.multiple_of(s * seg, seg), seg)
            a = dec[q, r, :]
            norm = nrm[q, r, :]
            ig = ing[q, r, :]
            rg = rec[q, r, :]
            m = mix[q, r, :]
            u = us[q, r, :] + ps[q, r, :] * cs[q, pl.ds(s, 1), :]
            state = gs[q, r, :] + qs[q, r, :] * rs[q, pl.ds(s, 1), :]
            im = ig * m
            hid = (u + norm * im).astype(BF16).astype(F32)
            grad_log = state * (u - im * (a * a) / norm)
            pab[r, lanes] = (grad_log * scale * (rg * (1.0 - rg))).astype(BF16)
            sn = state * norm
            pib[r, lanes] = (sn * im * (1.0 - ig)).astype(BF16)
            gm[q, r, :] = sn * ig
            z = gt[q, r, :]
            z2 = z * z
            t = jnp.tanh(GELU_C * (z + GELU_K * (z2 * z)))
            slope = 0.5 * (1.0 + t) + (0.5 * GELU_C) * z * (1.0 - t * t) * (
                1.0 + (3.0 * GELU_K) * z2
            )
            gg[r, lanes] = (og[r, lanes].astype(F32) * hid * slope).astype(BF16)
            return carry

        lax.fori_loop(0, SEGS, grads, 0)

    for g in range(chans // gw):
        cols = slice(g * gw, (g + 1) * gw)
        back = dot(pab[:, cols], bda[cols, :], ((1,), (1,)))
        back = back + dot(pib[:, cols], bdi[cols, :], ((1,), (1,)))
        for q in range(gw // LANES):
            at = g * (gw // LANES) + q
            gm[at, 0:rows, :] = gm[at, 0:rows, :] + back[:, q * LANES : (q + 1) * LANES]
    head = pltpu.make_async_remote_copy(
        src_ref=gm.at[:, pl.ds(0, 8), :], dst_ref=gm.at[:, pl.ds(rows, 8), :],
        send_sem=head_sem.at[0], recv_sem=head_sem.at[1],
        device_id={"sp": lax.rem(me + n_sp - 1, n_sp)}, device_id_type=MESH,
    )
    head.start()
    width = 512 if depth % 512 == 0 else depth
    for d in range(0, depth, width):
        acc[:, d : d + width] = dot(gg[...], wg[d : d + width, :], ((1,), (1,)))
    head.wait_recv()
    final = me == n_sp - 1
    for q in range(nq):
        gm[q, rows : rows + 8, :] = jnp.where(final, 0.0, gm[q, rows : rows + 8, :])
    for q in range(nq):
        lanes = slice(q * LANES, (q + 1) * LANES)
        for r in range(0, rows, step):
            total = jnp.zeros((step, LANES), F32)
            for j in range(taps_n):
                off = taps_n - 1 - j + r
                total = total + taps[j : j + 1, lanes] * gm[q, off : off + step, :]
            gb[r : r + step, lanes] = total.astype(BF16)

    order = list(range(1, last)) + [0]
    wide = depth // last
    share = depth // n_sp
    zi = me // per_last
    inner = lax.rem(me, per_last)

    def digit(i):
        return lax.rem(inner // (2**i), 2)

    def partner(i):
        return me + (1 - 2 * digit(i)) * (2**i)

    def stage_copy(i, k):
        size = 2 ** (bits - 1 - i)
        off = (1 - digit(i)) * size
        src = part.at[k, pl.ds(off, size)] if i == 0 else sacc.at[i - 1, k, pl.ds(off, size)]
        return pltpu.make_async_remote_copy(
            src_ref=src, dst_ref=srecv.at[i, k, pl.ds(0, size)],
            send_sem=ssend_sem.at[i, k], recv_sem=srecv_sem.at[i, k],
            device_id={"sp": partner(i)}, device_id_type=MESH,
        )

    def last_copy(k):
        src = part.at[k, 0] if bits == 0 else sacc.at[bits - 1, k, 0]
        return pltpu.make_async_remote_copy(
            src_ref=src, dst_ref=lrecv.at[k],
            send_sem=lsend_sem.at[k], recv_sem=lrecv_sem.at[k],
            device_id={"sp": lax.rem(zi + k, last) * per_last + inner}, device_id_type=MESH,
        )

    own = rows // n_tp
    pieces = tsend.shape[1]
    piece = depth // pieces

    def term(at, c):
        r = pl.ds(pl.multiple_of(at * own, own), own)
        cols = slice(c * piece, (c + 1) * piece)
        return acc[r, cols] + dot(gb[r, :], wx[cols, :], ((1,), (1,)))

    def term_copy(k, c):
        return pltpu.make_async_remote_copy(
            src_ref=tsend.at[k - 1, c], dst_ref=trecv.at[k - 1, c],
            send_sem=tsend_sem.at[k - 1, c], recv_sem=trecv_sem.at[k - 1, c],
            device_id={"tp": lax.rem(tp + k, n_tp)}, device_id_type=MESH,
        )

    def product(k):
        zd = lax.rem(zi + k, last)
        at = pl.ds(pl.multiple_of(zd * wide, wide), wide)
        prod = dot(xs[pl.ds(HALO, rows), at], gb[...], ((0,), (0,)))
        for v in range(per_last):
            part[k, bitrev(v, bits)] = prod[v * share : (v + 1) * share].astype(BF16)
        if bits:
            stage_copy(0, k).start()
        elif k:
            last_copy(k).start()

    def terms(c):
        for k in range(1, n_tp):
            tsend[k - 1, c] = term(lax.rem(tp + k, n_tp), c).astype(BF16)
            term_copy(k, c).start()

    terms(0)
    for k in order[:2]:
        product(k)
    for c in range(1, pieces):
        terms(c)
    for k in order[2:]:
        product(k)
    for i in range(bits):
        size = 2 ** (bits - 1 - i)
        for k in order:
            stage_copy(i, k).wait_recv()
            off = digit(i) * size
            for v in range(size):
                mine = part[k, off + v] if i == 0 else sacc[i - 1, k, off + v]
                sacc[i, k, v] = (mine.astype(F32) + srecv[i, k, v].astype(F32)).astype(BF16)
            if i + 1 < bits:
                stage_copy(i + 1, k).start()
            elif k:
                last_copy(k).start()
    for c in range(pieces):
        tsend[n_tp - 1, c] = term(tp, c).astype(BF16)
    total = (part[0, 0] if bits == 0 else sacc[bits - 1, 0, 0]).astype(F32)
    for k in range(1, last):
        last_copy(k).wait_recv()
        total = total + lrecv[k].astype(F32)
    gproj_out[...] = total
    for c in range(pieces):
        cols = slice(c * piece, (c + 1) * piece)
        total = tsend[n_tp - 1, c].astype(F32)
        for k in range(1, n_tp):
            term_copy(k, c).wait_recv()
            total = total + trecv[k - 1, c].astype(F32)
        gin_out[:, cols] = total.astype(BF16)

    halo.wait_send()
    head.wait_send()
    for c in sent:
        c.wait_send()
    for i in range(bits):
        for k in order:
            stage_copy(i, k).wait_send()
    for k in range(1, last):
        last_copy(k).wait_send()
    for c in range(pieces):
        for k in range(1, n_tp):
            term_copy(k, c).wait_send()


def body(n_sp, n_tp, block_input, proj_x, proj_gate, conv_taps, gate_a, gate_in, decay_param,
         log_jump, out_grad):
    rows, depth = block_input.shape
    chans = proj_x.shape[1]
    nq = chans // LANES
    gw = 256 if chans % 256 == 0 else LANES
    last, bits = factor(n_sp)
    per_last = n_sp // last
    share = depth // n_sp
    own = rows // n_tp
    pieces = 2
    stages = max(bits, 1)
    most = max(per_last // 2, 1)
    vm = pltpu.VMEM
    grid_f32 = vm((nq, rows, LANES), F32)
    dma = pltpu.SemaphoreType.DMA
    anywhere = pl.BlockSpec(memory_space=pl.ANY)
    local = pl.BlockSpec(memory_space=pltpu.VMEM)
    scratch = [
        vm((rows + HALO, depth), BF16), vm((depth, chans), BF16), vm((depth, chans), BF16),
        vm((rows, chans), F32), vm((rows, chans), BF16),
        grid_f32, vm((nq, rows + HALO, LANES), F32), grid_f32, vm((rows, chans), BF16),
        vm((chans, gw), BF16), vm((chans, gw), BF16),
        grid_f32, grid_f32, grid_f32, grid_f32, grid_f32, grid_f32, grid_f32, grid_f32,
        vm((nq, SEGS, LANES), F32), vm((nq, SEGS, LANES), F32),
        vm((2, 2 * nq, LANES), F32), vm((n_sp, 2 * nq, LANES), F32),
        vm((rows, chans), BF16), vm((rows, chans), BF16), vm((rows, chans), BF16),
        vm((nq, rows + 8, LANES), F32), vm((rows, chans), BF16), vm((rows, depth), F32),
        vm((n_tp, pieces, own, depth // pieces), BF16),
        vm((max(n_tp - 1, 1), pieces, own, depth // pieces), BF16),
        vm((last, per_last, share, chans), BF16),
        vm((stages, last, most, share, chans), BF16),
        vm((stages, last, most, share, chans), BF16),
        vm((last, share, chans), BF16),
        dma((5,)), dma((2,)), dma((n_sp,)), dma((n_sp,)), dma((2,)),
        dma((n_tp, pieces)), dma((n_tp, pieces)), dma((stages, last)), dma((stages, last)),
        dma((last,)), dma((last,)),
    ]
    return pl.pallas_call(
        functools.partial(kernel, n_sp, n_tp),
        out_shape=(
            jax.ShapeDtypeStruct((own, depth), BF16),
            jax.ShapeDtypeStruct((share, chans), F32),
        ),
        in_specs=[anywhere] * 3 + [local] * 4 + [anywhere] * 2,
        out_specs=(local, local),
        scratch_shapes=scratch,
        compiler_params=pltpu.CompilerParams(
            collective_id=0, has_side_effects=True, vmem_limit_bytes=56 * 1024 * 1024
        ),
    )(block_input, proj_x, proj_gate, conv_taps, gate_a, gate_in, decay_param.reshape(1, chans),
      log_jump, out_grad)


def solution(mesh):
    in_specs = (
        P("sp", None),
        P(None, "tp"),
        P(None, "tp"),
        P(None, "tp"),
        P("tp", None, None),
        P("tp", None, None),
        P("tp"),
        P("sp", "tp"),
        P("sp", "tp"),
    )
    out_specs = (P(("sp", "tp"), None), P("sp", "tp"))
    return jax.shard_map(
        functools.partial(body, mesh.shape["sp"], mesh.shape["tp"]),
        mesh=mesh, in_specs=in_specs, out_specs=out_specs, check_vma=False,
    )
```

```python
import functools

import jax
import jax.numpy as jnp
from jax import lax
from jax.experimental import pallas as pl
from jax.experimental.pallas import tpu as pltpu
from jax.sharding import PartitionSpec as P

gate_power = 8.0
LANES = 128
SEGS = 8
HALO = 16
GELU_C = 0.7978845608028654
GELU_K = 0.044715
F32 = jnp.float32
BF16 = jnp.bfloat16
MESH = pl.DeviceIdType.MESH


def neg_expm1(y, ey):
    p = 1.0 + y * (1.0 / 8.0)
    for k in range(7, 1, -1):
        p = 1.0 + y * (1.0 / k) * p
    return jnp.where(y > -0.5, -y * p, 1.0 - ey)


def log_sigmoid(x):
    e = jnp.exp(-jnp.abs(x))
    s = e / (2.0 + e)
    s2 = s * s
    p = jnp.full_like(s, 1.0 / 17.0)
    for k in range(15, 0, -2):
        p = p * s2 + 1.0 / k
    return jnp.minimum(x, 0.0) - 2.0 * s * p


def dot(a, b, dims=((1,), (0,))):
    return lax.dot_general(a, b, (dims, ((), ())), preferred_element_type=F32)


def factor(n):
    bits, last = 0, n
    while last > 4 and last % 2 == 0:
        last //= 2
        bits += 1
    return last, bits


def bitrev(v, bits):
    out = 0
    for i in range(bits):
        out = out * 2 + (v >> i) % 2
    return out


def kernel(
    n_sp, n_tp, x_hbm, wx_hbm, wg_hbm, taps_hbm, ga_hbm, gi_hbm, dp_hbm, lj_hbm, og_hbm,
    gin_out, gproj_out,
    taps, ga, gi, dp, xs, wx, wg, lj, og, gt, br, mix, mixb, bda, bdi, rec, ing, dec, nrm, us, ps, gs, qs,
    cs, rs, sbuf, rbuf, pab, pib, gg, gm, gb, acc, tsend, trecv, part, srecv, sacc, lrecv,
    loc_sem, halo_sem, msend_sem, mrecv_sem, head_sem, tsend_sem, trecv_sem, ssend_sem,
    srecv_sem, lsend_sem, lrecv_sem,
):
    me = lax.axis_index("sp")
    tp = lax.axis_index("tp")
    rows, chans = og.shape
    depth = wx.shape[0]
    nq = chans // LANES
    taps_n = taps.shape[0]
    block = ga.shape[1]
    seg = rows // SEGS
    last, bits = factor(n_sp)
    per_last = n_sp // last

    barrier = pltpu.get_barrier_semaphore()
    for k in range(1, n_sp):
        pl.semaphore_signal(
            barrier, inc=1, device_id={"sp": lax.rem(me + k, n_sp)}, device_id_type=MESH
        )
    for k in range(1, n_tp):
        pl.semaphore_signal(
            barrier, inc=1, device_id={"tp": lax.rem(tp + k, n_tp)}, device_id_type=MESH
        )
    loads = []
    for i, (src, dst) in enumerate(
        ((x_hbm, xs), (wg_hbm, wg), (wx_hbm, wx), (lj_hbm, lj), (og_hbm, og),
         (ga_hbm, ga), (gi_hbm, gi), (dp_hbm, dp), (taps_hbm, taps))
    ):
        c = pltpu.make_async_copy(src, dst, loc_sem.at[i])
        c.start()
        loads.append(c)

    gw = bda.shape[1]
    spread = (
        lax.rem(lax.broadcasted_iota(jnp.int32, (block, gw), 1), block)
        == lax.broadcasted_iota(jnp.int32, (block, gw), 0)
    ).astype(F32).astype(BF16)
    keep = lax.rem(lax.broadcasted_iota(jnp.int32, (chans, gw), 0), gw) // block == (
        lax.broadcasted_iota(jnp.int32, (chans, gw), 1) // block
    )

    loads[0].wait()
    loads[1].wait()
    pre = dot(xs[...], wg[...]).astype(BF16).astype(F32)
    for q in range(nq):
        gt[q] = pre[:, q * LANES : (q + 1) * LANES]
    loads[2].wait()
    pre = dot(xs[...], wx[...]).astype(BF16).astype(F32)
    for q in range(nq):
        br[q, HALO:, :] = pre[:, q * LANES : (q + 1) * LANES]
    for load in loads[3:]:
        load.wait()
    pl.semaphore_wait(barrier, n_sp - 1 + n_tp - 1)
    halo = pltpu.make_async_remote_copy(
        src_ref=br.at[:, pl.ds(rows + HALO - 8, 8), :], dst_ref=br.at[:, pl.ds(HALO - 8, 8), :],
        send_sem=halo_sem.at[0], recv_sem=halo_sem.at[1],
        device_id={"sp": lax.rem(me + 1, n_sp)}, device_id_type=MESH,
    )
    halo.start()
    for src, dst in ((ga, bda), (gi, bdi)):
        flat = src[...].reshape(chans, block)
        dst[...] = jnp.where(keep, dot(flat, spread), 0.0).astype(BF16)

    log_sig = log_sigmoid(dp[...])

    def convolve(r, step):
        for q in range(nq):
            lanes = slice(q * LANES, (q + 1) * LANES)
            total = jnp.zeros((step, LANES), F32)
            for j in range(taps_n):
                off = HALO - taps_n + 1 + j + r
                total = total + taps[j : j + 1, lanes] * br[q, off : off + step, :]
            half = total.astype(BF16)
            mixb[r : r + step, lanes] = half
            mix[q, r : r + step, :] = half.astype(F32)

    def gate_maps(r, count):
        for src, dst in ((bda, rec), (bdi, ing)):
            for g in range(chans // gw):
                cols = slice(g * gw, (g + 1) * gw)
                pre = dot(mixb[r : r + count, cols], src[cols, :])
                for q in range(gw // LANES):
                    dst[g * (gw // LANES) + q, r : r + count, :] = (
                        pre[:, q * LANES : (q + 1) * LANES]
                    )

    def gates(q, r):
        lanes = slice(q * LANES, (q + 1) * LANES)
        rg = jax.nn.sigmoid(rec[q, r, :])
        ig = jax.nn.sigmoid(ing[q, r, :])
        log_decay = rg * (gate_power * log_sig[:, lanes]) + lj[r, lanes]
        a = jnp.exp(log_decay)
        norm = jnp.sqrt(neg_expm1(2.0 * log_decay, a * a))
        rec[q, r, :] = rg
        ing[q, r, :] = ig
        dec[q, r, :] = a
        nrm[q, r, :] = norm
        us[q, r, :] = norm * ig * mix[q, r, :]

    sub = 64 if rows % 64 == 0 else rows
    step = 128 if rows % 128 == 0 else rows
    for q in range(nq):
        mix[q, 0:HALO, :] = jnp.zeros((HALO, LANES), F32)
        rec[q, 0:HALO, :] = jnp.zeros((HALO, LANES), F32)
        ing[q, 0:HALO, :] = jnp.zeros((HALO, LANES), F32)
    for r in range(HALO, rows, step):
        convolve(r, min(step, rows - r))
    gate_maps(HALO, rows - HALO)
    for q in range(nq):

        def most(i, carry, q=q):
            r = pl.ds(pl.multiple_of(i * sub, sub), sub)
            gates(q, r)
            z = gt[q, r, :]
            t = jnp.tanh(GELU_C * (z + GELU_K * (z * z * z)))
            gs[q, r, :] = og[r, q * LANES : (q + 1) * LANES].astype(F32) * (0.5 * z * (1.0 + t))
            return carry

        lax.fori_loop(0, rows // sub, most, 0)
    halo.wait_recv()
    first = me == 0
    for q in range(nq):
        br[q, HALO - 8 : HALO, :] = jnp.where(first, 0.0, br[q, HALO - 8 : HALO, :])
    convolve(0, HALO)
    gate_maps(0, HALO)
    for q in range(nq):
        gates(q, pl.ds(0, HALO))

    def scan(i, carry):
        out = []
        for q in range(nq):
            h, p, g, w = carry[q]
            f = pl.ds(i, SEGS, stride=seg)
            b = pl.ds(seg - 1 - i, SEGS, stride=seg)
            a = dec[q, f, :]
            u = a * h
            h = u + us[q, f, :]
            p = a * p
            us[q, f, :] = u
            ps[q, f, :] = p
            g = gs[q, b, :] + g
            gs[q, b, :] = g
            qs[q, b, :] = w
            a = dec[q, b, :]
            out.append((h, p, a * g, a * w))
        return tuple(out)

    zero = jnp.zeros((SEGS, LANES), F32)
    one = jnp.ones((SEGS, LANES), F32)
    ends = lax.fori_loop(0, seg, scan, tuple((zero, one, zero, one) for _ in range(nq)), unroll=2)
    for q in range(nq):
        h, p, g, _ = ends[q]
        fwd = jnp.zeros((1, LANES), F32)
        bwd = jnp.zeros((1, LANES), F32)
        prod = jnp.ones((1, LANES), F32)
        for s in range(SEGS):
            e = SEGS - 1 - s
            fwd = p[s : s + 1] * fwd + h[s : s + 1]
            bwd = p[e : e + 1] * bwd + g[e : e + 1]
            prod = prod * p[s : s + 1]
        sbuf[0, q : q + 1, :] = prod
        sbuf[1, q : q + 1, :] = prod
        sbuf[0, nq + q : nq + q + 1, :] = fwd
        sbuf[1, nq + q : nq + q + 1, :] = bwd

    sent = []
    for k in range(1, n_sp):
        peer = lax.rem(me + k, n_sp)
        c = pltpu.make_async_remote_copy(
            src_ref=sbuf.at[jnp.where(peer > me, 0, 1)], dst_ref=rbuf.at[k],
            send_sem=msend_sem.at[k], recv_sem=mrecv_sem.at[k],
            device_id={"sp": peer}, device_id_type=MESH,
        )
        c.start()
        sent.append(c)
    for q in range(nq):

        def ready(i, carry, q=q):
            r = pl.ds(pl.multiple_of(i * sub, sub), sub)
            lanes = slice(q * LANES, (q + 1) * LANES)
            a = dec[q, r, :]
            norm = nrm[q, r, :]
            ig = ing[q, r, :]
            rg = rec[q, r, :]
            im = ig * mix[q, r, :]
            drive = norm * im
            mix[q, r, :] = drive
            dec[q, r, :] = im * (a * a) / norm
            rec[q, r, :] = (gate_power * log_sig[:, lanes]) * (rg * (1.0 - rg))
            nrm[q, r, :] = drive * (1.0 - ig)
            ing[q, r, :] = norm * ig
            z = gt[q, r, :]
            z2 = z * z
            t = jnp.tanh(GELU_C * (z + GELU_K * (z2 * z)))
            slope = 0.5 * (1.0 + t) + (0.5 * GELU_C) * z * (1.0 - t * t) * (
                1.0 + (3.0 * GELU_K) * z2
            )
            gt[q, r, :] = og[r, lanes].astype(F32) * slope
            return carry

        lax.fori_loop(0, rows // sub, ready, 0)
    for c in sent:
        c.wait_recv()
    fwd = jnp.zeros((nq, LANES), F32)
    bwd = jnp.zeros((nq, LANES), F32)
    for k in range(n_sp - 1, 0, -1):
        fwd = jnp.where(me >= k, rbuf[k, 0:nq, :] * fwd + rbuf[k, nq : 2 * nq, :], fwd)
    for k in range(1, n_sp):
        bwd = jnp.where(me < k, rbuf[k, 0:nq, :] * bwd + rbuf[k, nq : 2 * nq, :], bwd)
    for q in range(nq):
        h, p, g, _ = ends[q]
        c = fwd[q : q + 1]
        d = bwd[q : q + 1]
        for s in range(SEGS):
            e = SEGS - 1 - s
            cs[q, s : s + 1, :] = c
            rs[q, e : e + 1, :] = d
            c = p[s : s + 1] * c + h[s : s + 1]
            d = p[e : e + 1] * d + g[e : e + 1]

    def grads(q, s):
        r = pl.ds(s * seg if isinstance(s, int) else pl.multiple_of(s * seg, seg), seg)
        lanes = slice(q * LANES, (q + 1) * LANES)
        u = us[q, r, :] + ps[q, r, :] * cs[q, pl.ds(s, 1), :]
        state = gs[q, r, :] + qs[q, r, :] * rs[q, pl.ds(s, 1), :]
        hid = (u + mix[q, r, :]).astype(BF16).astype(F32)
        pab[r, lanes] = (state * (u - dec[q, r, :]) * rec[q, r, :]).astype(BF16)
        pib[r, lanes] = (state * nrm[q, r, :]).astype(BF16)
        gm[q, r, :] = state * ing[q, r, :]
        gg[r, lanes] = (gt[q, r, :] * hid).astype(BF16)

    def back_maps(r, count):
        for g in range(chans // gw):
            cols = slice(g * gw, (g + 1) * gw)
            back = dot(pab[r : r + count, cols], bda[cols, :], ((1,), (1,)))
            back = back + dot(pib[r : r + count, cols], bdi[cols, :], ((1,), (1,)))
            for q in range(gw // LANES):
                at = g * (gw // LANES) + q
                gm[at, r : r + count, :] = (
                    gm[at, r : r + count, :] + back[:, q * LANES : (q + 1) * LANES]
                )

    for q in range(nq):
        grads(q, 0)
    back_maps(0, HALO)
    head = pltpu.make_async_remote_copy(
        src_ref=gm.at[:, pl.ds(0, 8), :], dst_ref=gm.at[:, pl.ds(rows, 8), :],
        send_sem=head_sem.at[0], recv_sem=head_sem.at[1],
        device_id={"sp": lax.rem(me + n_sp - 1, n_sp)}, device_id_type=MESH,
    )
    head.start()
    for q in range(nq):

        def others(s, carry, q=q):
            grads(q, s)
            return carry

        lax.fori_loop(1, SEGS, others, 0)
    back_maps(HALO, rows - HALO)
    width = 512 if depth % 512 == 0 else depth
    for d in range(0, depth, width):
        acc[:, d : d + width] = dot(gg[...], wg[d : d + width, :], ((1,), (1,)))
    head.wait_recv()
    final = me == n_sp - 1
    for q in range(nq):
        gm[q, rows : rows + 8, :] = jnp.where(final, 0.0, gm[q, rows : rows + 8, :])
    for q in range(nq):
        lanes = slice(q * LANES, (q + 1) * LANES)
        for r in range(0, rows, step):
            total = jnp.zeros((step, LANES), F32)
            for j in range(taps_n):
                off = taps_n - 1 - j + r
                total = total + taps[j : j + 1, lanes] * gm[q, off : off + step, :]
            gb[r : r + step, lanes] = total.astype(BF16)

    order = list(range(1, last)) + [0]
    wide = depth // last
    share = depth // n_sp
    zi = me // per_last
    inner = lax.rem(me, per_last)

    def digit(i):
        return lax.rem(inner // (2**i), 2)

    def partner(i):
        return me + (1 - 2 * digit(i)) * (2**i)

    def stage_copy(i, k):
        size = 2 ** (bits - 1 - i)
        off = (1 - digit(i)) * size
        src = part.at[k, pl.ds(off, size)] if i == 0 else sacc.at[i - 1, k, pl.ds(off, size)]
        return pltpu.make_async_remote_copy(
            src_ref=src, dst_ref=srecv.at[i, k, pl.ds(0, size)],
            send_sem=ssend_sem.at[i, k], recv_sem=srecv_sem.at[i, k],
            device_id={"sp": partner(i)}, device_id_type=MESH,
        )

    def last_copy(k):
        src = part.at[k, 0] if bits == 0 else sacc.at[bits - 1, k, 0]
        return pltpu.make_async_remote_copy(
            src_ref=src, dst_ref=lrecv.at[k],
            send_sem=lsend_sem.at[k], recv_sem=lrecv_sem.at[k],
            device_id={"sp": lax.rem(zi + k, last) * per_last + inner}, device_id_type=MESH,
        )

    own = rows // n_tp
    pieces = tsend.shape[1]
    piece = depth // pieces

    def term(at, c):
        r = pl.ds(pl.multiple_of(at * own, own), own)
        cols = slice(c * piece, (c + 1) * piece)
        return acc[r, cols] + dot(gb[r, :], wx[cols, :], ((1,), (1,)))

    def term_copy(k, c):
        return pltpu.make_async_remote_copy(
            src_ref=tsend.at[k - 1, c], dst_ref=trecv.at[k - 1, c],
            send_sem=tsend_sem.at[k - 1, c], recv_sem=trecv_sem.at[k - 1, c],
            device_id={"tp": lax.rem(tp + k, n_tp)}, device_id_type=MESH,
        )

    def product(k):
        zd = lax.rem(zi + k, last)
        at = pl.ds(pl.multiple_of(zd * wide, wide), wide)
        prod = dot(xs[:, at], gb[...], ((0,), (0,)))
        for v in range(per_last):
            part[k, bitrev(v, bits)] = prod[v * share : (v + 1) * share].astype(BF16)
        if bits:
            stage_copy(0, k).start()
        elif k:
            last_copy(k).start()

    def terms(c):
        for k in range(1, n_tp):
            tsend[k - 1, c] = term(lax.rem(tp + k, n_tp), c).astype(BF16)
            term_copy(k, c).start()

    def stage(i, k):
        size = 2 ** (bits - 1 - i)
        stage_copy(i, k).wait_recv()
        off = digit(i) * size
        for v in range(size):
            mine = part[k, off + v] if i == 0 else sacc[i - 1, k, off + v]
            sacc[i, k, v] = (mine.astype(F32) + srecv[i, k, v].astype(F32)).astype(BF16)
        if i + 1 < bits:
            stage_copy(i + 1, k).start()
        elif k:
            last_copy(k).start()

    todo = list(range(pieces))
    for n, k in enumerate(order):
        product(k)
        if todo:
            terms(todo.pop(0))
        if n and bits:
            stage(0, order[n - 1])
    for c in todo:
        terms(c)
    if bits:
        stage(0, order[-1])
    for i in range(1, bits):
        for k in order:
            stage(i, k)
    for c in range(pieces):
        tsend[n_tp - 1, c] = term(tp, c).astype(BF16)
    total = (part[0, 0] if bits == 0 else sacc[bits - 1, 0, 0]).astype(F32)
    for k in range(1, last):
        last_copy(k).wait_recv()
        total = total + lrecv[k].astype(F32)
    gproj_out[...] = total
    for c in range(pieces):
        cols = slice(c * piece, (c + 1) * piece)
        total = tsend[n_tp - 1, c].astype(F32)
        for k in range(1, n_tp):
            term_copy(k, c).wait_recv()
            total = total + trecv[k - 1, c].astype(F32)
        gin_out[:, cols] = total.astype(BF16)

    halo.wait_send()
    head.wait_send()
    for c in sent:
        c.wait_send()
    for i in range(bits):
        for k in order:
            stage_copy(i, k).wait_send()
    for k in range(1, last):
        last_copy(k).wait_send()
    for c in range(pieces):
        for k in range(1, n_tp):
            term_copy(k, c).wait_send()


def put_out(gin, gproj, gin_out, gproj_out, sem):
    one = pltpu.make_async_copy(gin, gin_out, sem.at[0])
    two = pltpu.make_async_copy(gproj, gproj_out, sem.at[1])
    one.start()
    two.start()
    one.wait()
    two.wait()


def body(n_sp, n_tp, block_input, proj_x, proj_gate, conv_taps, gate_a, gate_in, decay_param,
         log_jump, out_grad):
    rows, depth = block_input.shape
    chans = proj_x.shape[1]
    nq = chans // LANES
    gw = 256 if chans % 256 == 0 else LANES
    last, bits = factor(n_sp)
    per_last = n_sp // last
    share = depth // n_sp
    own = rows // n_tp
    pieces = 2
    stages = max(bits, 1)
    most = max(per_last // 2, 1)
    vm = pltpu.VMEM
    grid_f32 = vm((nq, rows, LANES), F32)
    dma = pltpu.SemaphoreType.DMA
    anywhere = pl.BlockSpec(memory_space=pl.ANY)
    local = pl.BlockSpec(memory_space=pltpu.VMEM)
    scratch = [
        vm(conv_taps.shape, F32), vm(gate_a.shape, BF16), vm(gate_in.shape, BF16), vm((1, chans), F32),
        vm((rows, depth), BF16), vm((depth, chans), BF16), vm((depth, chans), BF16),
        vm((rows, chans), F32), vm((rows, chans), BF16),
        grid_f32, vm((nq, rows + HALO, LANES), F32), grid_f32, vm((rows, chans), BF16),
        vm((chans, gw), BF16), vm((chans, gw), BF16),
        grid_f32, grid_f32, grid_f32, grid_f32, grid_f32, grid_f32, grid_f32, grid_f32,
        vm((nq, SEGS, LANES), F32), vm((nq, SEGS, LANES), F32),
        vm((2, 2 * nq, LANES), F32), vm((n_sp, 2 * nq, LANES), F32),
        vm((rows, chans), BF16), vm((rows, chans), BF16), vm((rows, chans), BF16),
        vm((nq, rows + 8, LANES), F32), vm((rows, chans), BF16), vm((rows, depth), F32),
        vm((n_tp, pieces, own, depth // pieces), BF16),
        vm((max(n_tp - 1, 1), pieces, own, depth // pieces), BF16),
        vm((last, per_last, share, chans), BF16),
        vm((stages, last, most, share, chans), BF16),
        vm((stages, last, most, share, chans), BF16),
        vm((last, share, chans), BF16),
        dma((9,)), dma((2,)), dma((n_sp,)), dma((n_sp,)), dma((2,)),
        dma((n_tp, pieces)), dma((n_tp, pieces)), dma((stages, last)), dma((stages, last)),
        dma((last,)), dma((last,)),
    ]
    held = pl.pallas_call(
        functools.partial(kernel, n_sp, n_tp),
        out_shape=(vm((own, depth), BF16), vm((share, chans), F32)),
        in_specs=[anywhere] * 9,
        out_specs=(local, local),
        scratch_shapes=scratch,
        compiler_params=pltpu.CompilerParams(
            collective_id=0, has_side_effects=True, vmem_limit_bytes=56 * 1024 * 1024
        ),
    )(block_input, proj_x, proj_gate, conv_taps, gate_a, gate_in, decay_param.reshape(1, chans),
      log_jump, out_grad)
    return pl.pallas_call(
        put_out,
        out_shape=(
            jax.ShapeDtypeStruct((own, depth), BF16),
            jax.ShapeDtypeStruct((share, chans), F32),
        ),
        in_specs=[local] * 2,
        out_specs=(anywhere, anywhere),
        scratch_shapes=[dma((2,))],
        compiler_params=pltpu.CompilerParams(vmem_limit_bytes=4 * 1024 * 1024),
    )(*held)


def solution(mesh):
    in_specs = (
        P("sp", None),
        P(None, "tp"),
        P(None, "tp"),
        P(None, "tp"),
        P("tp", None, None),
        P("tp", None, None),
        P("tp"),
        P("sp", "tp"),
        P("sp", "tp"),
    )
    out_specs = (P(("sp", "tp"), None), P("sp", "tp"))
    return jax.shard_map(
        functools.partial(body, mesh.shape["sp"], mesh.shape["tp"]),
        mesh=mesh, in_specs=in_specs, out_specs=out_specs, check_vma=False,
    )
```

```python
import functools

import jax
import jax.numpy as jnp
from jax import lax
from jax.experimental import pallas as pl
from jax.experimental.pallas import tpu as pltpu
from jax.sharding import PartitionSpec as P

gate_power = 8.0
LANES = 128
SEGS = 8
HALO = 16
GELU_C = 0.7978845608028654
GELU_K = 0.044715
F32 = jnp.float32
BF16 = jnp.bfloat16
MESH = pl.DeviceIdType.MESH


def neg_expm1(y, ey):
    p = 1.0 + y * (1.0 / 8.0)
    for k in range(7, 1, -1):
        p = 1.0 + y * (1.0 / k) * p
    return jnp.where(y > -0.5, -y * p, 1.0 - ey)


def log_sigmoid(x):
    e = jnp.exp(-jnp.abs(x))
    s = e / (2.0 + e)
    s2 = s * s
    p = jnp.full_like(s, 1.0 / 17.0)
    for k in range(15, 0, -2):
        p = p * s2 + 1.0 / k
    return jnp.minimum(x, 0.0) - 2.0 * s * p


def dot(a, b, dims=((1,), (0,))):
    return lax.dot_general(a, b, (dims, ((), ())), preferred_element_type=F32)


def factor(n):
    bits, last = 0, n
    while last > 4 and last % 2 == 0:
        last //= 2
        bits += 1
    return last, bits


def bitrev(v, bits):
    out = 0
    for i in range(bits):
        out = out * 2 + (v >> i) % 2
    return out


def kernel(
    n_sp, n_tp, x_hbm, wx_hbm, wg_hbm, taps_hbm, ga_hbm, gi_hbm, dp_hbm, lj_hbm, og_hbm,
    gin_out, gproj_out,
    taps, ga, gi, dp, xs, wx, wg, lj, og, gt, br, mix, mixb, bda, bdi, rec, ing, dec, nrm, us, ps, gs, qs,
    cs, rs, sbuf, rbuf, pab, pib, gg, gm, gb, wgt, wxt, xt, tsend, trecv, part, srecv, sacc, lrecv,
    loc_sem, halo_sem, msend_sem, mrecv_sem, head_sem, tsend_sem, trecv_sem, ssend_sem,
    srecv_sem, lsend_sem, lrecv_sem,
):
    me = lax.axis_index("sp")
    tp = lax.axis_index("tp")
    rows, chans = og.shape
    depth = wx.shape[0]
    nq = chans // LANES
    taps_n = taps.shape[0]
    block = ga.shape[1]
    seg = rows // SEGS
    last, bits = factor(n_sp)
    per_last = n_sp // last

    barrier = pltpu.get_barrier_semaphore()
    for k in range(1, n_sp):
        pl.semaphore_signal(
            barrier, inc=1, device_id={"sp": lax.rem(me + k, n_sp)}, device_id_type=MESH
        )
    for k in range(1, n_tp):
        pl.semaphore_signal(
            barrier, inc=1, device_id={"tp": lax.rem(tp + k, n_tp)}, device_id_type=MESH
        )
    loads = []
    for i, (src, dst) in enumerate(
        ((x_hbm, xs), (wg_hbm, wg), (wx_hbm, wx), (lj_hbm, lj), (og_hbm, og),
         (ga_hbm, ga), (gi_hbm, gi), (dp_hbm, dp), (taps_hbm, taps))
    ):
        c = pltpu.make_async_copy(src, dst, loc_sem.at[i])
        c.start()
        loads.append(c)

    gw = bda.shape[1]
    spread = (
        lax.rem(lax.broadcasted_iota(jnp.int32, (block, gw), 1), block)
        == lax.broadcasted_iota(jnp.int32, (block, gw), 0)
    ).astype(F32).astype(BF16)
    keep = lax.rem(lax.broadcasted_iota(jnp.int32, (chans, gw), 0), gw) // block == (
        lax.broadcasted_iota(jnp.int32, (chans, gw), 1) // block
    )

    loads[0].wait()
    loads[1].wait()
    pre = dot(xs[...], wg[...]).astype(BF16).astype(F32)
    for q in range(nq):
        gt[q] = pre[:, q * LANES : (q + 1) * LANES]
    loads[2].wait()
    pre = dot(xs[...], wx[...]).astype(BF16).astype(F32)
    for q in range(nq):
        br[q, HALO:, :] = pre[:, q * LANES : (q + 1) * LANES]
    for load in loads[3:]:
        load.wait()
    pl.semaphore_wait(barrier, n_sp - 1 + n_tp - 1)
    halo = pltpu.make_async_remote_copy(
        src_ref=br.at[:, pl.ds(rows + HALO - 8, 8), :], dst_ref=br.at[:, pl.ds(HALO - 8, 8), :],
        send_sem=halo_sem.at[0], recv_sem=halo_sem.at[1],
        device_id={"sp": lax.rem(me + 1, n_sp)}, device_id_type=MESH,
    )
    halo.start()
    for src, dst in ((ga, bda), (gi, bdi)):
        flat = src[...].reshape(chans, block)
        dst[...] = jnp.where(keep, dot(flat, spread), 0.0).astype(BF16)

    log_sig = log_sigmoid(dp[...])

    def convolve(r, step):
        for q in range(nq):
            lanes = slice(q * LANES, (q + 1) * LANES)
            total = jnp.zeros((step, LANES), F32)
            for j in range(taps_n):
                off = HALO - taps_n + 1 + j + r
                total = total + taps[j : j + 1, lanes] * br[q, off : off + step, :]
            half = total.astype(BF16)
            mixb[r : r + step, lanes] = half
            mix[q, r : r + step, :] = half.astype(F32)

    def gate_maps(r, count):
        for src, dst in ((bda, rec), (bdi, ing)):
            for g in range(chans // gw):
                cols = slice(g * gw, (g + 1) * gw)
                pre = dot(mixb[r : r + count, cols], src[cols, :])
                for q in range(gw // LANES):
                    dst[g * (gw // LANES) + q, r : r + count, :] = (
                        pre[:, q * LANES : (q + 1) * LANES]
                    )

    def gates(q, r):
        lanes = slice(q * LANES, (q + 1) * LANES)
        rg = jax.nn.sigmoid(rec[q, r, :])
        ig = jax.nn.sigmoid(ing[q, r, :])
        log_decay = rg * (gate_power * log_sig[:, lanes]) + lj[r, lanes]
        a = jnp.exp(log_decay)
        norm = jnp.sqrt(neg_expm1(2.0 * log_decay, a * a))
        rec[q, r, :] = rg
        ing[q, r, :] = ig
        dec[q, r, :] = a
        nrm[q, r, :] = norm
        us[q, r, :] = norm * ig * mix[q, r, :]

    sub = 64 if rows % 64 == 0 else rows
    step = 128 if rows % 128 == 0 else rows
    for q in range(nq):
        mix[q, 0:HALO, :] = jnp.zeros((HALO, LANES), F32)
        rec[q, 0:HALO, :] = jnp.zeros((HALO, LANES), F32)
        ing[q, 0:HALO, :] = jnp.zeros((HALO, LANES), F32)
    for r in range(HALO, rows, step):
        convolve(r, min(step, rows - r))
    gate_maps(HALO, rows - HALO)
    for q in range(nq):

        def most(i, carry, q=q):
            r = pl.ds(pl.multiple_of(i * sub, sub), sub)
            gates(q, r)
            z = gt[q, r, :]
            t = jnp.tanh(GELU_C * (z + GELU_K * (z * z * z)))
            gs[q, r, :] = og[r, q * LANES : (q + 1) * LANES].astype(F32) * (0.5 * z * (1.0 + t))
            return carry

        lax.fori_loop(0, rows // sub, most, 0)
    halo.wait_recv()
    first = me == 0
    for q in range(nq):
        br[q, HALO - 8 : HALO, :] = jnp.where(first, 0.0, br[q, HALO - 8 : HALO, :])
    convolve(0, HALO)
    gate_maps(0, HALO)
    for q in range(nq):
        gates(q, pl.ds(0, HALO))

    def scan(i, carry):
        out = []
        for q in range(nq):
            h, p, g, w = carry[q]
            f = pl.ds(i, SEGS, stride=seg)
            b = pl.ds(seg - 1 - i, SEGS, stride=seg)
            a = dec[q, f, :]
            u = a * h
            h = u + us[q, f, :]
            p = a * p
            us[q, f, :] = u
            ps[q, f, :] = p
            g = gs[q, b, :] + g
            gs[q, b, :] = g
            qs[q, b, :] = w
            a = dec[q, b, :]
            out.append((h, p, a * g, a * w))
        return tuple(out)

    zero = jnp.zeros((SEGS, LANES), F32)
    one = jnp.ones((SEGS, LANES), F32)
    ends = lax.fori_loop(0, seg, scan, tuple((zero, one, zero, one) for _ in range(nq)), unroll=4)
    for q in range(nq):
        h, p, g, _ = ends[q]
        fwd = jnp.zeros((1, LANES), F32)
        bwd = jnp.zeros((1, LANES), F32)
        prod = jnp.ones((1, LANES), F32)
        for s in range(SEGS):
            e = SEGS - 1 - s
            fwd = p[s : s + 1] * fwd + h[s : s + 1]
            bwd = p[e : e + 1] * bwd + g[e : e + 1]
            prod = prod * p[s : s + 1]
        sbuf[0, q : q + 1, :] = prod
        sbuf[1, q : q + 1, :] = prod
        sbuf[0, nq + q : nq + q + 1, :] = fwd
        sbuf[1, nq + q : nq + q + 1, :] = bwd

    sent = []
    for k in range(1, n_sp):
        peer = lax.rem(me + k, n_sp)
        c = pltpu.make_async_remote_copy(
            src_ref=sbuf.at[jnp.where(peer > me, 0, 1)], dst_ref=rbuf.at[k],
            send_sem=msend_sem.at[k], recv_sem=mrecv_sem.at[k],
            device_id={"sp": peer}, device_id_type=MESH,
        )
        c.start()
        sent.append(c)
    for q in range(nq):

        def ready(i, carry, q=q):
            r = pl.ds(pl.multiple_of(i * sub, sub), sub)
            lanes = slice(q * LANES, (q + 1) * LANES)
            a = dec[q, r, :]
            norm = nrm[q, r, :]
            ig = ing[q, r, :]
            rg = rec[q, r, :]
            im = ig * mix[q, r, :]
            drive = norm * im
            mix[q, r, :] = drive
            dec[q, r, :] = im * (a * a) / norm
            rec[q, r, :] = (gate_power * log_sig[:, lanes]) * (rg * (1.0 - rg))
            nrm[q, r, :] = drive * (1.0 - ig)
            ing[q, r, :] = norm * ig
            z = gt[q, r, :]
            z2 = z * z
            t = jnp.tanh(GELU_C * (z + GELU_K * (z2 * z)))
            slope = 0.5 * (1.0 + t) + (0.5 * GELU_C) * z * (1.0 - t * t) * (
                1.0 + (3.0 * GELU_K) * z2
            )
            gt[q, r, :] = og[r, lanes].astype(F32) * slope
            return carry

        lax.fori_loop(0, rows // sub, ready, 0)
    wgt[...] = wg[...].T
    wxt[...] = wx[...].T
    xt[...] = xs[...].T
    for c in sent:
        c.wait_recv()
    fwd = jnp.zeros((nq, LANES), F32)
    bwd = jnp.zeros((nq, LANES), F32)
    for k in range(n_sp - 1, 0, -1):
        fwd = jnp.where(me >= k, rbuf[k, 0:nq, :] * fwd + rbuf[k, nq : 2 * nq, :], fwd)
    for k in range(1, n_sp):
        bwd = jnp.where(me < k, rbuf[k, 0:nq, :] * bwd + rbuf[k, nq : 2 * nq, :], bwd)
    for q in range(nq):
        h, p, g, _ = ends[q]
        c = fwd[q : q + 1]
        d = bwd[q : q + 1]
        for s in range(SEGS):
            e = SEGS - 1 - s
            cs[q, s : s + 1, :] = c
            rs[q, e : e + 1, :] = d
            c = p[s : s + 1] * c + h[s : s + 1]
            d = p[e : e + 1] * d + g[e : e + 1]

    def grads(q, s):
        r = pl.ds(s * seg if isinstance(s, int) else pl.multiple_of(s * seg, seg), seg)
        lanes = slice(q * LANES, (q + 1) * LANES)
        u = us[q, r, :] + ps[q, r, :] * cs[q, pl.ds(s, 1), :]
        state = gs[q, r, :] + qs[q, r, :] * rs[q, pl.ds(s, 1), :]
        hid = (u + mix[q, r, :]).astype(BF16).astype(F32)
        pab[r, lanes] = (state * (u - dec[q, r, :]) * rec[q, r, :]).astype(BF16)
        pib[r, lanes] = (state * nrm[q, r, :]).astype(BF16)
        gm[q, r, :] = state * ing[q, r, :]
        gg[r, lanes] = (gt[q, r, :] * hid).astype(BF16)

    def back_maps(r, count):
        for g in range(chans // gw):
            cols = slice(g * gw, (g + 1) * gw)
            back = dot(pab[r : r + count, cols], bda[cols, :], ((1,), (1,)))
            back = back + dot(pib[r : r + count, cols], bdi[cols, :], ((1,), (1,)))
            for q in range(gw // LANES):
                at = g * (gw // LANES) + q
                gm[at, r : r + count, :] = (
                    gm[at, r : r + count, :] + back[:, q * LANES : (q + 1) * LANES]
                )

    for q in range(nq):
        grads(q, 0)
    back_maps(0, HALO)
    head = pltpu.make_async_remote_copy(
        src_ref=gm.at[:, pl.ds(0, 8), :], dst_ref=gm.at[:, pl.ds(rows, 8), :],
        send_sem=head_sem.at[0], recv_sem=head_sem.at[1],
        device_id={"sp": lax.rem(me + n_sp - 1, n_sp)}, device_id_type=MESH,
    )
    head.start()
    for q in range(nq):

        def others(s, carry, q=q):
            grads(q, s)
            return carry

        lax.fori_loop(1, SEGS, others, 0)
    back_maps(HALO, rows - HALO)
    def convolve_back(r, end):
        for q in range(nq):
            lanes = slice(q * LANES, (q + 1) * LANES)
            total = jnp.zeros((end - r, LANES), F32)
            for j in range(taps_n):
                off = taps_n - 1 - j
                total = total + taps[j : j + 1, lanes] * gm[q, r + off : end + off, :]
            gb[r:end, lanes] = total.astype(BF16)

    own = rows // n_tp
    pieces = tsend.shape[1]
    piece = own // pieces

    def term(at, c):
        r = pl.ds(pl.multiple_of(at * own + c * piece, piece), piece)
        return dot(gg[r, :], wgt[...]) + dot(gb[r, :], wxt[...])

    def term_copy(k, c):
        return pltpu.make_async_remote_copy(
            src_ref=tsend.at[k - 1, c], dst_ref=trecv.at[k - 1, c],
            send_sem=tsend_sem.at[k - 1, c], recv_sem=trecv_sem.at[k - 1, c],
            device_id={"tp": lax.rem(tp + k, n_tp)}, device_id_type=MESH,
        )

    def terms(c):
        for k in range(1, n_tp):
            tsend[k - 1, c] = term(lax.rem(tp + k, n_tp), c).astype(BF16)
            term_copy(k, c).start()

    todo = list(range(pieces))
    for r in range(0, rows - HALO, step):
        convolve_back(r, min(r + step, rows - HALO))
    if pieces > 1:
        terms(todo.pop(0))
    head.wait_recv()
    final = me == n_sp - 1
    for q in range(nq):
        gm[q, rows : rows + 8, :] = jnp.where(final, 0.0, gm[q, rows : rows + 8, :])
    convolve_back(rows - HALO, rows)

    order = list(range(1, last)) + [0]
    wide = depth // last
    share = depth // n_sp
    zi = me // per_last
    inner = lax.rem(me, per_last)

    def digit(i):
        return lax.rem(inner // (2**i), 2)

    def partner(i):
        return me + (1 - 2 * digit(i)) * (2**i)

    def stage_copy(i, k):
        size = 2 ** (bits - 1 - i)
        off = (1 - digit(i)) * size
        src = part.at[k, pl.ds(off, size)] if i == 0 else sacc.at[i - 1, k, pl.ds(off, size)]
        return pltpu.make_async_remote_copy(
            src_ref=src, dst_ref=srecv.at[i, k, pl.ds(0, size)],
            send_sem=ssend_sem.at[i, k], recv_sem=srecv_sem.at[i, k],
            device_id={"sp": partner(i)}, device_id_type=MESH,
        )

    def last_copy(k):
        src = part.at[k, 0] if bits == 0 else sacc.at[bits - 1, k, 0]
        return pltpu.make_async_remote_copy(
            src_ref=src, dst_ref=lrecv.at[k],
            send_sem=lsend_sem.at[k], recv_sem=lrecv_sem.at[k],
            device_id={"sp": lax.rem(zi + k, last) * per_last + inner}, device_id_type=MESH,
        )

    def product(k):
        zd = lax.rem(zi + k, last)
        at = pl.ds(pl.multiple_of(zd * wide, wide), wide)
        prod = dot(xt[at, :], gb[...])
        for v in range(per_last):
            part[k, bitrev(v, bits)] = prod[v * share : (v + 1) * share].astype(BF16)
        if bits:
            stage_copy(0, k).start()
        elif k:
            last_copy(k).start()

    def stage(i, k):
        size = 2 ** (bits - 1 - i)
        stage_copy(i, k).wait_recv()
        off = digit(i) * size
        for v in range(size):
            mine = part[k, off + v] if i == 0 else sacc[i - 1, k, off + v]
            sacc[i, k, v] = (mine.astype(F32) + srecv[i, k, v].astype(F32)).astype(BF16)
        if i + 1 < bits:
            stage_copy(i + 1, k).start()
        elif k:
            last_copy(k).start()

    for n, k in enumerate(order):
        product(k)
        if n and bits:
            stage(0, order[n - 1])
    if bits:
        stage(0, order[-1])
    for c in todo:
        terms(c)
    mine = list(range(pieces))
    for i in range(1, bits):
        for k in order:
            stage(i, k)
            if mine:
                c = mine.pop(0)
                tsend[n_tp - 1, c] = term(tp, c).astype(BF16)
    for c in mine:
        tsend[n_tp - 1, c] = term(tp, c).astype(BF16)
    total = (part[0, 0] if bits == 0 else sacc[bits - 1, 0, 0]).astype(F32)
    for k in range(1, last):
        last_copy(k).wait_recv()
        total = total + lrecv[k].astype(F32)
    gproj_out[...] = total
    for c in range(pieces):
        total = tsend[n_tp - 1, c].astype(F32)
        for k in range(1, n_tp):
            term_copy(k, c).wait_recv()
            total = total + trecv[k - 1, c].astype(F32)
        gin_out[c * piece : (c + 1) * piece, :] = total.astype(BF16)

    halo.wait_send()
    head.wait_send()
    for c in sent:
        c.wait_send()
    for i in range(bits):
        for k in order:
            stage_copy(i, k).wait_send()
    for k in range(1, last):
        last_copy(k).wait_send()
    for c in range(pieces):
        for k in range(1, n_tp):
            term_copy(k, c).wait_send()


def put_out(gin, gproj, gin_out, gproj_out, sem):
    one = pltpu.make_async_copy(gin, gin_out, sem.at[0])
    two = pltpu.make_async_copy(gproj, gproj_out, sem.at[1])
    one.start()
    two.start()
    one.wait()
    two.wait()


def body(n_sp, n_tp, block_input, proj_x, proj_gate, conv_taps, gate_a, gate_in, decay_param,
         log_jump, out_grad):
    rows, depth = block_input.shape
    chans = proj_x.shape[1]
    nq = chans // LANES
    gw = 256 if chans % 256 == 0 else LANES
    last, bits = factor(n_sp)
    per_last = n_sp // last
    share = depth // n_sp
    own = rows // n_tp
    pieces = 2 if own % 32 == 0 else 1
    stages = max(bits, 1)
    most = max(per_last // 2, 1)
    vm = pltpu.VMEM
    grid_f32 = vm((nq, rows, LANES), F32)
    dma = pltpu.SemaphoreType.DMA
    anywhere = pl.BlockSpec(memory_space=pl.ANY)
    local = pl.BlockSpec(memory_space=pltpu.VMEM)
    scratch = [
        vm(conv_taps.shape, F32), vm(gate_a.shape, BF16), vm(gate_in.shape, BF16), vm((1, chans), F32),
        vm((rows, depth), BF16), vm((depth, chans), BF16), vm((depth, chans), BF16),
        vm((rows, chans), F32), vm((rows, chans), BF16),
        grid_f32, vm((nq, rows + HALO, LANES), F32), grid_f32, vm((rows, chans), BF16),
        vm((chans, gw), BF16), vm((chans, gw), BF16),
        grid_f32, grid_f32, grid_f32, grid_f32, grid_f32, grid_f32, grid_f32, grid_f32,
        vm((nq, SEGS, LANES), F32), vm((nq, SEGS, LANES), F32),
        vm((2, 2 * nq, LANES), F32), vm((n_sp, 2 * nq, LANES), F32),
        vm((rows, chans), BF16), vm((rows, chans), BF16), vm((rows, chans), BF16),
        vm((nq, rows + 8, LANES), F32), vm((rows, chans), BF16),
        vm((chans, depth), BF16), vm((chans, depth), BF16), vm((depth, rows), BF16),
        vm((n_tp, pieces, own // pieces, depth), BF16),
        vm((max(n_tp - 1, 1), pieces, own // pieces, depth), BF16),
        vm((last, per_last, share, chans), BF16),
        vm((stages, last, most, share, chans), BF16),
        vm((stages, last, most, share, chans), BF16),
        vm((last, share, chans), BF16),
        dma((9,)), dma((2,)), dma((n_sp,)), dma((n_sp,)), dma((2,)),
        dma((n_tp, pieces)), dma((n_tp, pieces)), dma((stages, last)), dma((stages, last)),
        dma((last,)), dma((last,)),
    ]
    held = pl.pallas_call(
        functools.partial(kernel, n_sp, n_tp),
        out_shape=(vm((own, depth), BF16), vm((share, chans), F32)),
        in_specs=[anywhere] * 9,
        out_specs=(local, local),
        scratch_shapes=scratch,
        compiler_params=pltpu.CompilerParams(
            collective_id=0, has_side_effects=True, vmem_limit_bytes=56 * 1024 * 1024
        ),
    )(block_input, proj_x, proj_gate, conv_taps, gate_a, gate_in, decay_param.reshape(1, chans),
      log_jump, out_grad)
    return pl.pallas_call(
        put_out,
        out_shape=(
            jax.ShapeDtypeStruct((own, depth), BF16),
            jax.ShapeDtypeStruct((share, chans), F32),
        ),
        in_specs=[local] * 2,
        out_specs=(anywhere, anywhere),
        scratch_shapes=[dma((2,))],
        compiler_params=pltpu.CompilerParams(vmem_limit_bytes=4 * 1024 * 1024),
    )(*held)


def solution(mesh):
    in_specs = (
        P("sp", None),
        P(None, "tp"),
        P(None, "tp"),
        P(None, "tp"),
        P("tp", None, None),
        P("tp", None, None),
        P("tp"),
        P("sp", "tp"),
        P("sp", "tp"),
    )
    out_specs = (P(("sp", "tp"), None), P("sp", "tp"))
    return jax.shard_map(
        functools.partial(body, mesh.shape["sp"], mesh.shape["tp"]),
        mesh=mesh, in_specs=in_specs, out_specs=out_specs, check_vma=False,
    )
```
